32 devices in a mesh: ep: 8 (over z, x), tp: 4 (over y, core).
Axes of the slice: x: 2, y: 2, z: 4, core: 2. Of those that a mesh axis runs over, the one named last changes fastest.
Arguments:
- tokens: bfloat16 [64, 2048], P('ep', 'tp'), may hold values from -10 to 10, as said below
- norm_gain: float32 [2048], P('tp'), may hold values from 0.5 to 1.5
- norm_bias: float32 [2048], P('tp'), may hold values from -0.3 to 0.3
- group_pick: int32 [64, 1], P('ep'), may hold values from 0 to 1; in each aligned block of 8 rows (0 to 7, 8 to 15, ...) at most 4 rows name the same one
- member_pick: int32 [64, 4], P('ep'), may hold values from 0 to 7, all different within a row
- picked_probs: float32 [64, 4], P('ep'), may hold values from 0.05 to 1
- gate_weight: bfloat16 [16, 2048, 1024], P('ep', 'tp'), may hold values from -0.125 to 0.125
- up_weight: bfloat16 [16, 2048, 1024], P('ep', 'tp'), may hold values from -0.125 to 0.125
- down_weight: bfloat16 [16, 1024, 2048], P('ep', None, 'tp'), may hold values from -0.375 to 0.375
Outputs:
- mixed: bfloat16 [64, 2048], P('ep', 'tp')
The draws below stay inside these ranges and needn't reach their ends.
Inputs may be any that keep to these rules, and one draw needn't show every extreme that they name: `group_pick`: each entry is a group number from 0 to 1; within each aligned block of 8 tokens no group is named by more than 4 tokens, a bound that some block reaches. `member_pick`: each token's 4 entries are different member numbers from 0 to 7. `tokens`: each token is its own offset between -2 and 2 plus its own scale between 0.25 and 2 times entries of at most 4 in size.
All inputs are finite; a program needn't handle non-finite values.
Results may differ from the reference program's by a relative error of at most 0.01.
Values may be sent and summed in bfloat16 or wider, within the bound.
A program may use at most 64 MiB of HBM per device.

```python
import math
import jax
import jax.numpy as jnp
import numpy as np
from jax import lax

D = 2048
FF = 1024
EPG = 8
TOP_K = 4
TOK_DEV = 8
TOKENS = 64
EXPERTS = 16
GROUPS = 2
GCAP = 4


def draw_tokens(key, part):
    offset_key, scale_key, noise_key = jax.random.split(key, 3)
    offsets = jax.random.uniform(offset_key, (TOKENS, 1), jnp.float32, -2.0, 2.0)
    logs = jax.random.uniform(scale_key, (TOKENS, 1), jnp.float32, math.log(0.5), math.log(2.0))
    noise = jnp.clip(jax.random.normal(noise_key, (TOKENS, D), jnp.float32), -4.0, 4.0)
    return (offsets + jnp.exp(logs) * noise).astype(jnp.bfloat16)


def level_of(key, extent, cuts, smallest, largest):
    def one(dim, parts):
        heights = jax.random.uniform(jax.random.fold_in(jax.random.fold_in(key, 6), dim), (parts,), jnp.float32, smallest / len(cuts), largest / len(cuts))
        return jnp.repeat(jnp.exp(heights), extent[dim] // parts).reshape((-1,) + (1,) * (len(extent) - dim - 1))

    factor_of = one(*cuts[0])
    for cut in cuts[1:]:
        factor_of = factor_of * one(*cut)
    return factor_of


def picks_of(stream_key, rows, count, top, lift):
    sequence = jax.random.permutation(jax.random.fold_in(stream_key, 1), count)
    favour = sequence
    for power in range(3):
        favour = favour * favour // count
    favour = favour * lift // count
    tickets = jax.random.randint(jax.random.fold_in(stream_key, 2), (rows, count), 0, 4096) + favour
    fixed_rows = jax.random.permutation(jax.random.fold_in(stream_key, 3), rows)[jnp.arange(count) % rows]
    tickets = jnp.where(jnp.arange(rows)[:, None] == fixed_rows[None, :], 1 << 14, tickets)
    score = tickets * count + jnp.arange(count)
    return lax.top_k(score.astype(jnp.int32), top)[1].astype(jnp.int32)


def routed_block(stream_key, own, number, rows, number_of, top, most, lean):
    ranking = jax.random.permutation(stream_key, number_of)
    heavy_load, usual = portions_of(number_of, rows * top, most, lean, True), portions_of(number_of, rows * top, most, lean, False)
    places = jnp.arange(number_of)

    def named(tallies, turn):
        used = int((tallies > 0).sum())
        fixed = max(1, used // 4)
        moved = fixed + (places - fixed + turn * (used - fixed)) % max(1, number_of - fixed)
        return jnp.zeros((number_of,), jnp.int32).at[ranking[jnp.where(places < fixed, places, moved)]].set(jnp.asarray(tallies, jnp.int32))

    tallies = jnp.where(number % 4 == 0, named(heavy_load, number // 4), named(usual, number - number // 4 - 1))
    mixed = jax.random.permutation(jax.random.fold_in(own, 3), number_of)
    source_of, sink = mixed[0:number_of // 2 * 2:2], mixed[1:number_of // 2 * 2:2]
    room = jnp.minimum(tallies[source_of] - 1, most - tallies[sink]) // 2
    room = jnp.where((source_of == ranking[0]) | (sink == ranking[0]) | (tallies[sink] == 0), 0, jnp.maximum(room, 0))
    moved = jax.random.randint(jax.random.fold_in(own, 4), (number_of // 2,), 0, 1 << 20) % (room + 1)
    tallies = tallies.at[source_of].add(-moved).at[sink].add(moved)
    items = jnp.searchsorted(jnp.cumsum(tallies), jnp.arange(rows * top), side="right").astype(jnp.int32)
    grid = items.reshape(top, rows).T
    grid = grid[jax.random.permutation(jax.random.fold_in(own, 1), rows)]
    turn = jax.random.randint(jax.random.fold_in(own, 2), (rows, 1), 0, top)
    return jnp.take_along_axis(grid, (jnp.arange(top)[None, :] + turn) % top, axis=1)


def portions_of(amount, total, bound, lean, full):
    portions = [(1 << 20) // math.isqrt(standing ** lean) + 1 for standing in range(1, amount + 1)]
    largest = bound if full else min(bound, max(-(-total // amount), total * portions[0] // sum(portions)))
    least = 1 if total - largest >= amount - 1 else 0
    given, surplus = [largest] + [least] * (amount - 1), total - largest - least * (amount - 1)
    while surplus > 0:
        free = [i for i in range(1, amount) if given[i] < largest] or [i for i in range(1, amount) if given[i] < bound]
        whole, left = sum([portions[i] for i in free]), surplus
        for i in free:
            extra = min(bound - given[i], max(1, left * portions[i] // whole), surplus)
            given[i] = given[i] + extra
            surplus = surplus - extra
    return np.array(given)


def scatter_about(stream_key, dims, scale, limit, cuts=(), held_as=jnp.bfloat16):
    factor_of = level_of(stream_key, dims, cuts, -0.22, 0.18) if cuts else 1.0
    drawn = jax.random.normal(stream_key, dims, jnp.float32) * scale * factor_of
    return jnp.minimum(jnp.maximum(drawn, -limit), limit).astype(held_as)


def setup_inputs(seed: int = 0) -> dict:
    arg_keys = jax.random.split(jax.random.key(seed), 10)
    tokens = draw_tokens(jax.random.fold_in(arg_keys[9], 71), 0)
    norm_gain = jnp.clip(1.0 + 0.1 * jax.random.normal(arg_keys[1], (D,), jnp.float32), 0.5, 1.5)
    norm_bias = scatter_about(arg_keys[2], (D,), 0.1, 0.3, ((0, 4),), jnp.float32)
    group_pick_keys = jax.random.split(jax.random.fold_in(arg_keys[3], 1), TOKENS // TOK_DEV)
    group_pick_turns = jax.random.permutation(jax.random.fold_in(arg_keys[3], 3), TOKENS // TOK_DEV)
    group_pick = jax.vmap(lambda own, number: routed_block(jax.random.fold_in(arg_keys[3], 2), own, number, TOK_DEV, GROUPS, 1, GCAP, 2))(group_pick_keys, group_pick_turns).reshape((TOKENS, 1))
    member_pick = picks_of(arg_keys[4], TOKENS, EPG, TOP_K, 4096)
    picked_probs = jnp.clip(jnp.exp(math.log(1.0) - 2.9957323 * jax.random.uniform(arg_keys[5], (TOKENS, TOP_K), jnp.float32) ** level_of(arg_keys[5], (TOKENS, TOP_K), ((0, 8),), -0.2, 0.2)), 0.05, 1.0)
    gate_weight = scatter_about(arg_keys[6], (EXPERTS, D, FF), D ** -0.5, 0.125, ((0, 8), (1, 4)))
    up_weight = scatter_about(arg_keys[7], (EXPERTS, D, FF), D ** -0.5, 0.125, ((0, 8), (1, 4)))
    down_weight = scatter_about(arg_keys[8], (EXPERTS, FF, D), (FF // 4) ** -0.5, 0.375, ((0, 8), (2, 4)))
    return {"tokens": tokens, "norm_gain": norm_gain, "norm_bias": norm_bias, "group_pick": group_pick, "member_pick": member_pick, "picked_probs": picked_probs, "gate_weight": gate_weight, "up_weight": up_weight, "down_weight": down_weight}


norm_epsilon = 1e-5


def reference(tokens, norm_gain, norm_bias, group_pick, member_pick, picked_probs, gate_weight, up_weight, down_weight):
    values = tokens.astype(jnp.float32)
    center = jnp.mean(values, axis=1, keepdims=True)
    shifted = values - center
    spread = jnp.mean(shifted * shifted, axis=1, keepdims=True)
    scaled = shifted * lax.rsqrt(spread + norm_epsilon)
    normed = (scaled * norm_gain.astype(jnp.float32) + norm_bias.astype(jnp.float32)).astype(jnp.bfloat16)
    chosen = (group_pick * EPG + member_pick).astype(jnp.int32)
    shares = picked_probs / jnp.sum(picked_probs, axis=1, keepdims=True)

    def one_token(packed):
        row, picks, weights = packed
        row_wide = row.astype(jnp.float32)
        gate_rows = jnp.take(gate_weight, picks, axis=0).astype(jnp.float32)
        up_rows = jnp.take(up_weight, picks, axis=0).astype(jnp.float32)
        down_rows = jnp.take(down_weight, picks, axis=0).astype(jnp.float32)
        gate_sum = jnp.einsum("d,kdf->kf", row_wide, gate_rows)
        up_sum = jnp.einsum("d,kdf->kf", row_wide, up_rows)
        hidden = (jax.nn.silu(gate_sum) * up_sum).astype(jnp.bfloat16)
        expert_out = jnp.einsum("kf,kfd->kd", hidden.astype(jnp.float32), down_rows).astype(jnp.bfloat16)
        return jnp.sum(weights[:, None] * expert_out.astype(jnp.float32), axis=0)

    combined = lax.map(one_token, (normed, chosen, shares))
    return combined.astype(jnp.bfloat16)
```

```python
import functools

import jax
import jax.numpy as jnp
from jax import lax
from jax.experimental import pallas as pl
from jax.experimental.pallas import tpu as pltpu
from jax.sharding import PartitionSpec as P

EPG = 8
CORES = 2
LANES = 128
norm_epsilon = 1e-05
MESH = pl.DeviceIdType.MESH
F32 = jnp.float32
BF16 = jnp.bfloat16


def iota(shape, dim):
    return lax.broadcasted_iota(jnp.int32, shape, dim)


def kernel(
    E, T, G, cap,
    tokens_h, gain_h, bias_h, group_h, member_h, probs_h, gate_h, up_h, down_h,
    out_ref,
    tokens_v, gain_v, bias_v, group_v, member_v, probs_v, gate_v, up_v, down_v,
    stat_buf, share_out, share_in, share_all, rows_out, rows_in, rows_all,
    core_out, core_in, y_out, y_in, held, hid_own, hid_other, back_out, back_in,
    local_sem, weight_sem,
    stat_s, stat_r, share_s, share_r, rows_s, rows_r,
    core_s, core_r, y_s, y_r, hid_s, hid_r, back_s, back_r,
):
    n, width = tokens_h.shape
    LE = gate_h.shape[0]
    FF = gate_h.shape[2]
    half = FF // CORES
    NY = T // CORES
    S = G * cap
    R = E * cap
    group_devices = EPG // LE
    me = lax.axis_index("ep")
    mt = lax.axis_index("tp")
    core = lax.rem(mt, CORES)
    my = lax.div(mt, CORES)

    def ep_at(d):
        return lax.rem(me + d, E)

    def tp_at(d):
        return lax.rem(mt + d, T)

    def remote(src, dst, ssem, rsem, ep, tp):
        return pltpu.make_async_remote_copy(
            src_ref=src, dst_ref=dst, send_sem=ssem, recv_sem=rsem,
            device_id=(ep, tp), device_id_type=MESH,
        )

    barrier = pltpu.get_barrier_semaphore()
    for d in range(1, E):
        pl.semaphore_signal(barrier, inc=1, device_id=(ep_at(d), mt), device_id_type=MESH)
    for d in range(1, T):
        pl.semaphore_signal(barrier, inc=1, device_id=(me, tp_at(d)), device_id_type=MESH)

    small = [
        pltpu.make_async_copy(h, v, local_sem.at[i])
        for i, (h, v) in enumerate(
            ((group_h, group_v), (member_h, member_v), (probs_h, probs_v),
             (tokens_h, tokens_v), (gain_h, gain_v), (bias_h, bias_v))
        )
    ]
    for c in small:
        c.start()
    weights = [
        [pltpu.make_async_copy(h.at[j], v.at[j], weight_sem.at[w, j]) for j in range(LE)]
        for w, (h, v) in enumerate(((gate_h, gate_v), (up_h, up_v), (down_h, down_v)))
    ]
    for w in range(2):
        for j in range(LE):
            weights[w][j].start()
    for j in range(LE):
        weights[2][j].start()
    for c in small:
        c.wait()

    lane = iota((n, LANES), 1)
    sub = iota((n, LANES), 0)
    group = group_v[...].astype(F32)
    group_wide = jnp.broadcast_to(group, (n, LANES))
    group_row = jnp.sum(jnp.where(lane == sub, group_wide, 0.0), axis=0, keepdims=True)
    same = jnp.where(group_wide == group_row, 1.0, 0.0)
    slot_row = jnp.sum(jnp.where(sub < lane, same, 0.0), axis=0, keepdims=True)
    slot_col = jnp.sum(jnp.where(lane < sub, same, 0.0), axis=1, keepdims=True)
    key_row = jnp.where(iota((1, LANES), 1) < n, group_row * cap + slot_row, -1.0)
    key_col = group * cap + slot_col
    place = jnp.where(key_row == iota((S, LANES), 0).astype(F32), 1.0, 0.0)

    def pack(v):
        total = place[:, 0:1] * v[0:1, :]
        for t in range(1, n):
            total += place[:, t : t + 1] * v[t : t + 1, :]
        return total

    probs = probs_v[...]
    member = member_v[...]
    shares = probs / jnp.sum(probs, axis=1, keepdims=True)
    share_tile = jnp.zeros((n, LANES), F32)
    for k in range(probs.shape[1]):
        share_tile += jnp.where(lane == member[:, k : k + 1], shares[:, k : k + 1], 0.0)
    share_tile = pack(share_tile)
    for g in range(G):
        share_out[g] = share_tile[g * cap : (g + 1) * cap, :]

    values = pack(tokens_v[...].astype(F32))
    center_here = jnp.sum(values, axis=1, keepdims=True) / width
    away = values - center_here
    square_here = jnp.sum(away * away, axis=1, keepdims=True)
    slane = iota((S, LANES), 1)
    stat_buf[0] = jnp.where(slane == 0, center_here, jnp.where(slane == 1, square_here, 0.0))

    pl.semaphore_wait(barrier, E + T - 2)

    stat = [
        remote(stat_buf.at[0], stat_buf.at[d], stat_s.at[d - 1], stat_r.at[d - 1], me, tp_at(d))
        for d in range(1, T)
    ]
    for c in stat:
        c.start()
    share = []
    for d in range(1, E):
        p = ep_at(d)
        c = remote(
            share_out.at[lax.div(p, group_devices)], share_in.at[d],
            share_s.at[d - 1], share_r.at[d - 1], p, mt,
        )
        c.start()
        share.append(c)
    share_in[0] = share_out[lax.div(me, group_devices)]
    gain = gain_v[...]
    bias = bias_v[...]
    for c in stat:
        c.wait_recv()
    stats = [stat_buf[d] for d in range(T)]
    center = sum(s[:, 0:1] for s in stats) / T
    square = sum(s[:, 1:2] + width * (s[:, 0:1] - center) * (s[:, 0:1] - center) for s in stats)
    spread = square / (width * T)
    normed = (values - center) * lax.rsqrt(spread + norm_epsilon) * gain + bias
    for g in range(G):
        rows_out[g] = normed[g * cap : (g + 1) * cap, :].astype(BF16)

    sent = []
    for d in range(1, E):
        p = ep_at(d)
        c = remote(
            rows_out.at[lax.div(p, group_devices)], rows_in.at[d],
            rows_s.at[d - 1], rows_r.at[d - 1], p, mt,
        )
        c.start()
        sent.append(c)
    rows_in[0] = rows_out[lax.div(me, group_devices)]
    rows_all[0:cap, :] = rows_in[0].astype(F32)
    for w in range(2):
        for j in range(LE):
            weights[w][j].wait()
    for d in range(1, E):
        sent[d - 1].wait_recv()
        rows_all[d * cap : (d + 1) * cap, :] = rows_in[d].astype(F32)
    rows = rows_all[...].astype(BF16)

    mine = pl.ds(pl.multiple_of(core * half, half), half)
    theirs = pl.ds(pl.multiple_of((1 - core) * half, half), half)
    partner = my * CORES + (1 - core)
    to_core = []
    for j in range(LE):
        for w, v in enumerate((gate_v, up_v)):
            core_out[j, w] = jnp.dot(rows, v[j, :, theirs], preferred_element_type=F32).astype(BF16)
        c = remote(core_out.at[j], core_in.at[j], core_s.at[j], core_r.at[j], me, partner)
        c.start()
        to_core.append(c)
    to_y = []
    for j in range(LE):
        for w, v in enumerate((gate_v, up_v)):
            held[j, w] = jnp.dot(rows, v[j, :, mine], preferred_element_type=F32)
        to_core[j].wait_recv()
        for w in range(2):
            total = held[j, w] + core_in[j, w].astype(F32)
            held[j, w] = total
            y_out[j, w] = total.astype(BF16)
        copies = []
        for d in range(1, NY):
            c = remote(
                y_out.at[j], y_in.at[j, d - 1], y_s.at[j, d - 1], y_r.at[j, d - 1],
                me, lax.rem(my + d, NY) * CORES + core,
            )
            c.start()
            copies.append(c)
        to_y.append(copies)
    for d in range(1, E):
        share[d - 1].wait_recv()
    for d in range(E):
        share_all[d * cap : (d + 1) * cap, :] = share_in[d]
    for j in range(LE):
        weights[2][j].wait()
    to_hid = []
    partial = []
    for j in range(LE):
        gate = held[j, 0]
        up = held[j, 1]
        for d in range(1, NY):
            to_y[j][d - 1].wait_recv()
            gate += y_in[j, d - 1, 0].astype(F32)
            up += y_in[j, d - 1, 1].astype(F32)
        hidden = (gate / (1.0 + jnp.exp(-gate)) * up).astype(BF16)
        hid_own[j] = hidden
        c = remote(hid_own.at[j], hid_other.at[j], hid_s.at[j], hid_r.at[j], me, partner)
        c.start()
        to_hid.append(c)
        partial.append(jnp.dot(hidden, down_v[j, mine, :], preferred_element_type=F32))
    total = jnp.zeros((R, width), F32)
    rlane = iota((R, LANES), 1)
    weight_tile = share_all[...]
    for j in range(LE):
        to_hid[j].wait_recv()
        expert = partial[j] + jnp.dot(hid_other[j], down_v[j, theirs, :], preferred_element_type=F32)
        which = lax.rem(me * LE + j, EPG)
        weight = jnp.sum(jnp.where(rlane == which, weight_tile, 0.0), axis=1, keepdims=True)
        total += weight * expert.astype(BF16).astype(F32)

    back = []
    for d in range(1, E):
        back_out[d] = total[d * cap : (d + 1) * cap, :].astype(BF16)
        c = remote(
            back_out.at[d], back_in.at[me], back_s.at[d - 1], back_r.at[d - 1],
            lax.rem(me - d + E, E), mt,
        )
        c.start()
        back.append(c)
    back_in[me] = total[0:cap, :].astype(BF16)
    for c in stat:
        c.wait_send()
    for c in share:
        c.wait_send()
    for c in sent:
        c.wait_send()
    for j in range(LE):
        to_core[j].wait_send()
        to_hid[j].wait_send()
        for c in to_y[j]:
            c.wait_send()
    for c in back:
        c.wait()
    finder = jnp.where(key_col == lane.astype(F32), 1.0, 0.0)
    mixed = jnp.zeros((n, width), F32)
    for g in range(G):
        part = back_in[g * group_devices].astype(F32)
        for p in range(1, group_devices):
            part += back_in[g * group_devices + p].astype(F32)
        for s in range(cap):
            at = g * cap + s
            mixed += finder[:, at : at + 1] * part[s : s + 1, :]
    out_ref[...] = mixed.astype(BF16)


def per_device(E, T, tokens, norm_gain, norm_bias, group_pick, member_pick, picked_probs,
               gate_weight, up_weight, down_weight):
    n, width = tokens.shape
    LE, _, FF = gate_weight.shape
    half = FF // CORES
    NY = T // CORES
    G = LE * E // EPG
    cap = max(n // 4, (n + G - 1) // G)
    S = G * cap
    R = E * cap
    k = picked_probs.shape[1]
    dma = pltpu.SemaphoreType.DMA
    V = pltpu.VMEM
    scratch = [
        V((n, width), BF16), V((1, width), F32), V((1, width), F32),
        V((n, 1), jnp.int32), V((n, k), jnp.int32), V((n, k), F32),
        V((LE, width, FF), BF16), V((LE, width, FF), BF16), V((LE, FF, width), BF16),
        V((T, S, LANES), F32),
        V((G, cap, LANES), F32), V((E, cap, LANES), F32), V((R, LANES), F32),
        V((G, cap, width), BF16), V((E, cap, width), BF16), V((R, width), F32),
        V((LE, 2, R, half), BF16), V((LE, 2, R, half), BF16),
        V((LE, 2, R, half), BF16), V((LE, NY - 1, 2, R, half), BF16),
        V((LE, 2, R, half), F32),
        V((LE, R, half), BF16), V((LE, R, half), BF16),
        V((E, cap, width), BF16), V((E, cap, width), BF16),
        dma((6,)), dma((3, LE)),
        dma((T - 1,)), dma((T - 1,)), dma((E - 1,)), dma((E - 1,)), dma((E - 1,)), dma((E - 1,)),
        dma((LE,)), dma((LE,)), dma((LE, NY - 1)), dma((LE, NY - 1)), dma((LE,)), dma((LE,)),
        dma((E - 1,)), dma((E - 1,)),
    ]
    anywhere = pl.BlockSpec(memory_space=pl.ANY)
    return pl.pallas_call(
        functools.partial(kernel, E, T, G, cap),
        out_shape=jax.ShapeDtypeStruct((n, width), BF16),
        in_specs=[anywhere] * 9,
        out_specs=pl.BlockSpec(memory_space=pltpu.VMEM),
        scratch_shapes=scratch,
        compiler_params=pltpu.CompilerParams(collective_id=0, has_side_effects=True),
        name="moe_step",
    )(tokens, norm_gain.reshape(1, width), norm_bias.reshape(1, width), group_pick, member_pick,
      picked_probs, gate_weight, up_weight, down_weight)


def solution(mesh):
    placed = (
        P("ep", "tp"), P("tp"), P("tp"), P("ep", None), P("ep", None), P("ep", None),
        P("ep", "tp", None), P("ep", "tp", None), P("ep", None, "tp"),
    )
    body = functools.partial(per_device, mesh.shape["ep"], mesh.shape["tp"])
    return jax.shard_map(body, mesh=mesh, in_specs=placed, out_specs=P("ep", "tp"), check_vma=False)
```

```python
import functools

import jax
import jax.numpy as jnp
from jax import lax
from jax.experimental import pallas as pl
from jax.experimental.pallas import tpu as pltpu
from jax.sharding import PartitionSpec as P

EPG = 8
CORES = 2
LANES = 128
norm_epsilon = 1e-05
MESH = pl.DeviceIdType.MESH
F32 = jnp.float32
BF16 = jnp.bfloat16


def iota(shape, dim):
    return lax.broadcasted_iota(jnp.int32, shape, dim)


def kernel(
    E, T, G, cap,
    tokens_h, gain_h, bias_h, group_h, member_h, probs_h, gate_h, up_h, down_h,
    out_ref,
    tokens_v, gain_v, bias_v, group_v, member_v, probs_v, gate_v, up_v, down_v,
    stat_buf, share_out, share_in, share_all, rows_out, rows_in, rows_all,
    core_out, core_in, y_out, y_in, held, hid_own, hid_other, back_out, back_in,
    local_sem, weight_sem,
    stat_s, stat_r, share_s, share_r, rows_s, rows_r,
    core_s, core_r, y_s, y_r, hid_s, hid_r, back_s, back_r,
):
    n, width = tokens_h.shape
    LE = gate_h.shape[0]
    FF = gate_h.shape[2]
    half = FF // CORES
    NY = T // CORES
    S = G * cap
    R = E * cap
    group_devices = EPG // LE
    me = lax.axis_index("ep")
    mt = lax.axis_index("tp")
    core = lax.rem(mt, CORES)
    my = lax.div(mt, CORES)

    def ep_at(d):
        return lax.rem(me + d, E)

    def tp_at(d):
        return lax.rem(mt + d, T)

    def remote(src, dst, ssem, rsem, ep, tp):
        return pltpu.make_async_remote_copy(
            src_ref=src, dst_ref=dst, send_sem=ssem, recv_sem=rsem,
            device_id=(ep, tp), device_id_type=MESH,
        )

    barrier = pltpu.get_barrier_semaphore()
    for d in range(1, E):
        pl.semaphore_signal(barrier, inc=1, device_id=(ep_at(d), mt), device_id_type=MESH)
    for d in range(1, T):
        pl.semaphore_signal(barrier, inc=1, device_id=(me, tp_at(d)), device_id_type=MESH)

    small = [
        pltpu.make_async_copy(h, v, local_sem.at[i])
        for i, (h, v) in enumerate(
            ((group_h, group_v), (member_h, member_v), (probs_h, probs_v),
             (tokens_h, tokens_v), (gain_h, gain_v), (bias_h, bias_v))
        )
    ]
    for c in small:
        c.start()
    weights = [
        [pltpu.make_async_copy(h.at[j], v.at[j], weight_sem.at[w, j]) for j in range(LE)]
        for w, (h, v) in enumerate(((gate_h, gate_v), (up_h, up_v), (down_h, down_v)))
    ]
    for w in range(2):
        for j in range(LE):
            weights[w][j].start()
    for j in range(LE):
        weights[2][j].start()
    for c in small:
        c.wait()

    lane = iota((n, n), 1)
    sub = iota((n, n), 0)

    def column(row):
        wide = jnp.broadcast_to(row, (n, n))
        return jnp.sum(jnp.where(lane == sub, wide, 0.0), axis=1, keepdims=True)

    group_row = group_v[...].astype(F32)
    group_col = column(group_row)
    same = jnp.where(group_col == group_row, 1.0, 0.0)
    slot_row = jnp.sum(jnp.where(sub < lane, same, 0.0), axis=0, keepdims=True)
    slot_col = jnp.sum(jnp.where(lane < sub, same, 0.0), axis=1, keepdims=True)
    key_row = group_row * cap + slot_row
    key_col = group_col * cap + slot_col
    place = jnp.where(key_row == iota((S, n), 0).astype(F32), 1.0, 0.0)

    def pack(v):
        total = place[:, 0:1] * v[0:1, :]
        for t in range(1, n):
            total += place[:, t : t + 1] * v[t : t + 1, :]
        return total

    probs = probs_v[...]
    member = member_v[...].astype(F32)
    shares = probs / jnp.sum(probs, axis=0, keepdims=True)
    share_lane = iota((n, LANES), 1).astype(F32)
    share_tile = jnp.zeros((n, LANES), F32)
    for k in range(probs.shape[0]):
        hit = share_lane == column(member[k : k + 1, :])
        share_tile += jnp.where(hit, column(shares[k : k + 1, :]), 0.0)
    share_tile = pack(share_tile)
    for g in range(G):
        share_out[g] = share_tile[g * cap : (g + 1) * cap, :]

    values = pack(tokens_v[...].astype(F32))
    center_here = jnp.sum(values, axis=1, keepdims=True) / width
    away = values - center_here
    square_here = jnp.sum(away * away, axis=1, keepdims=True)
    slane = iota((S, LANES), 1)
    stat_buf[0] = jnp.where(slane == 0, center_here, jnp.where(slane == 1, square_here, 0.0))

    pl.semaphore_wait(barrier, E + T - 2)

    stat = [
        remote(stat_buf.at[0], stat_buf.at[d], stat_s.at[d - 1], stat_r.at[d - 1], me, tp_at(d))
        for d in range(1, T)
    ]
    for c in stat:
        c.start()
    share = []
    for d in range(1, E):
        p = ep_at(d)
        c = remote(
            share_out.at[lax.div(p, group_devices)], share_in.at[d],
            share_s.at[d - 1], share_r.at[d - 1], p, mt,
        )
        c.start()
        share.append(c)
    share_in[0] = share_out[lax.div(me, group_devices)]
    gain = gain_v[...]
    bias = bias_v[...]
    for c in stat:
        c.wait_recv()
    stats = [stat_buf[d] for d in range(T)]
    center = sum(s[:, 0:1] for s in stats) / T
    square = sum(s[:, 1:2] + width * (s[:, 0:1] - center) * (s[:, 0:1] - center) for s in stats)
    spread = square / (width * T)
    normed = (values - center) * lax.rsqrt(spread + norm_epsilon) * gain + bias
    for g in range(G):
        rows_out[g] = normed[g * cap : (g + 1) * cap, :].astype(BF16)

    sent = []
    for d in range(1, E):
        p = ep_at(d)
        c = remote(
            rows_out.at[lax.div(p, group_devices)], rows_in.at[d],
            rows_s.at[d - 1], rows_r.at[d - 1], p, mt,
        )
        c.start()
        sent.append(c)
    rows_in[0] = rows_out[lax.div(me, group_devices)]
    rows_all[0:cap, :] = rows_in[0].astype(F32)
    for w in range(2):
        for j in range(LE):
            weights[w][j].wait()
    for d in range(1, E):
        sent[d - 1].wait_recv()
        rows_all[d * cap : (d + 1) * cap, :] = rows_in[d].astype(F32)
    rows = rows_all[...].astype(BF16)

    mine = pl.ds(pl.multiple_of(core * half, half), half)
    theirs = pl.ds(pl.multiple_of((1 - core) * half, half), half)
    partner = my * CORES + (1 - core)
    to_core = []
    for j in range(LE):
        for w, v in enumerate((gate_v, up_v)):
            core_out[j, w] = jnp.dot(rows, v[j, :, theirs], preferred_element_type=F32).astype(BF16)
        c = remote(core_out.at[j], core_in.at[j], core_s.at[j], core_r.at[j], me, partner)
        c.start()
        to_core.append(c)
    to_y = []
    for j in range(LE):
        for w, v in enumerate((gate_v, up_v)):
            held[j, w] = jnp.dot(rows, v[j, :, mine], preferred_element_type=F32)
        to_core[j].wait_recv()
        for w in range(2):
            total = held[j, w] + core_in[j, w].astype(F32)
            held[j, w] = total
            y_out[j, w] = total.astype(BF16)
        copies = []
        for d in range(1, NY):
            c = remote(
                y_out.at[j], y_in.at[j, d - 1], y_s.at[j, d - 1], y_r.at[j, d - 1],
                me, lax.rem(my + d, NY) * CORES + core,
            )
            c.start()
            copies.append(c)
        to_y.append(copies)
    for d in range(1, E):
        share[d - 1].wait_recv()
    for d in range(E):
        share_all[d * cap : (d + 1) * cap, :] = share_in[d]
    for j in range(LE):
        weights[2][j].wait()
    to_hid = []
    partial = []
    for j in range(LE):
        gate = held[j, 0]
        up = held[j, 1]
        for d in range(1, NY):
            to_y[j][d - 1].wait_recv()
            gate += y_in[j, d - 1, 0].astype(F32)
            up += y_in[j, d - 1, 1].astype(F32)
        hidden = (gate / (1.0 + jnp.exp(-gate)) * up).astype(BF16)
        hid_own[j] = hidden
        c = remote(hid_own.at[j], hid_other.at[j], hid_s.at[j], hid_r.at[j], me, partner)
        c.start()
        to_hid.append(c)
        partial.append(jnp.dot(hidden, down_v[j, mine, :], preferred_element_type=F32))
    total = jnp.zeros((R, width), F32)
    rlane = iota((R, LANES), 1)
    weight_tile = share_all[...]
    for j in range(LE):
        to_hid[j].wait_recv()
        expert = partial[j] + jnp.dot(hid_other[j], down_v[j, theirs, :], preferred_element_type=F32)
        which = lax.rem(me * LE + j, EPG)
        weight = jnp.sum(jnp.where(rlane == which, weight_tile, 0.0), axis=1, keepdims=True)
        total += weight * expert.astype(BF16).astype(F32)

    back = []
    for d in range(1, E):
        back_out[d] = total[d * cap : (d + 1) * cap, :].astype(BF16)
        c = remote(
            back_out.at[d], back_in.at[me], back_s.at[d - 1], back_r.at[d - 1],
            lax.rem(me - d + E, E), mt,
        )
        c.start()
        back.append(c)
    back_in[me] = total[0:cap, :].astype(BF16)
    for c in stat:
        c.wait_send()
    for c in share:
        c.wait_send()
    for c in sent:
        c.wait_send()
    for j in range(LE):
        to_core[j].wait_send()
        to_hid[j].wait_send()
        for c in to_y[j]:
            c.wait_send()
    for c in back:
        c.wait()
    finder = jnp.where(key_col == iota((n, LANES), 1).astype(F32), 1.0, 0.0)
    mixed = jnp.zeros((n, width), F32)
    for g in range(G):
        part = back_in[g * group_devices].astype(F32)
        for p in range(1, group_devices):
            part += back_in[g * group_devices + p].astype(F32)
        for s in range(cap):
            at = g * cap + s
            mixed += finder[:, at : at + 1] * part[s : s + 1, :]
    out_ref[...] = mixed


def per_device(E, T, tokens, norm_gain, norm_bias, group_pick, member_pick, picked_probs,
               gate_weight, up_weight, down_weight):
    n, width = tokens.shape
    LE, _, FF = gate_weight.shape
    half = FF // CORES
    NY = T // CORES
    G = LE * E // EPG
    cap = max(n // 4, (n + G - 1) // G)
    S = G * cap
    R = E * cap
    k = picked_probs.shape[1]
    dma = pltpu.SemaphoreType.DMA
    V = pltpu.VMEM
    scratch = [
        V((n, width), BF16), V((1, width), F32), V((1, width), F32),
        V((1, n), jnp.int32), V((k, n), jnp.int32), V((k, n), F32),
        V((LE, width, FF), BF16), V((LE, width, FF), BF16), V((LE, FF, width), BF16),
        V((T, S, LANES), F32),
        V((G, cap, LANES), F32), V((E, cap, LANES), F32), V((R, LANES), F32),
        V((G, cap, width), BF16), V((E, cap, width), BF16), V((R, width), F32),
        V((LE, 2, R, half), BF16), V((LE, 2, R, half), BF16),
        V((LE, 2, R, half), BF16), V((LE, NY - 1, 2, R, half), BF16),
        V((LE, 2, R, half), F32),
        V((LE, R, half), BF16), V((LE, R, half), BF16),
        V((E, cap, width), BF16), V((E, cap, width), BF16),
        dma((6,)), dma((3, LE)),
        dma((T - 1,)), dma((T - 1,)), dma((E - 1,)), dma((E - 1,)), dma((E - 1,)), dma((E - 1,)),
        dma((LE,)), dma((LE,)), dma((LE, NY - 1)), dma((LE, NY - 1)), dma((LE,)), dma((LE,)),
        dma((E - 1,)), dma((E - 1,)),
    ]
    anywhere = pl.BlockSpec(memory_space=pltpu.HBM)
    combined = pl.pallas_call(
        functools.partial(kernel, E, T, G, cap),
        out_shape=jax.ShapeDtypeStruct((n, width), F32),
        in_specs=[anywhere] * 9,
        out_specs=pl.BlockSpec(memory_space=pltpu.VMEM),
        scratch_shapes=scratch,
        compiler_params=pltpu.CompilerParams(collective_id=0, has_side_effects=True, vmem_limit_bytes=32 * 1024 * 1024),
        name="moe_step",
    )(tokens, norm_gain.reshape(1, width), norm_bias.reshape(1, width), group_pick.T, member_pick.T,
      picked_probs.T, gate_weight, up_weight, down_weight)
    return combined.astype(BF16)


def solution(mesh):
    placed = (
        P("ep", "tp"), P("tp"), P("tp"), P("ep", None), P("ep", None), P("ep", None),
        P("ep", "tp", None), P("ep", "tp", None), P("ep", None, "tp"),
    )
    body = functools.partial(per_device, mesh.shape["ep"], mesh.shape["tp"])
    return jax.shard_map(body, mesh=mesh, in_specs=placed, out_specs=P("ep", "tp"), check_vma=False)
```

```python
import functools

import jax
import jax.numpy as jnp
from jax import lax
from jax.experimental import pallas as pl
from jax.experimental.pallas import tpu as pltpu
from jax.sharding import PartitionSpec as P

EPG = 8
CORES = 2
LANES = 128
norm_epsilon = 1e-05
MESH = pl.DeviceIdType.MESH
F32 = jnp.float32
BF16 = jnp.bfloat16


def iota(shape, dim):
    return lax.broadcasted_iota(jnp.int32, shape, dim)


def kernel(
    E, T, G, cap,
    tokens_h, gain_h, bias_h, group_h, member_h, probs_h, gate_h, up_h, down_h,
    out_ref,
    tokens_v, gain_v, bias_v, group_v, member_v, probs_v, gate_v, up_v, down_v,
    stat_buf, share_out, share_in, share_all, rows_out, rows_in, rows_all,
    core_out, core_in, y_out, y_in, held, hid_own, hid_other, back_out, back_in,
    local_sem, weight_sem,
    stat_s, stat_r, share_s, share_r, rows_s, rows_r,
    core_s, core_r, y_s, y_r, hid_s, hid_r, back_s, back_r,
):
    n, width = tokens_h.shape
    LE = gate_h.shape[0]
    FF = gate_h.shape[2]
    half = FF // CORES
    NY = T // CORES
    S = G * cap
    R = E * cap
    group_devices = EPG // LE
    me = lax.axis_index("ep")
    mt = lax.axis_index("tp")
    core = lax.rem(mt, CORES)
    my = lax.div(mt, CORES)

    def ep_at(d):
        return lax.rem(me + d, E)

    def tp_at(d):
        return lax.rem(mt + d, T)

    def remote(src, dst, ssem, rsem, ep, tp):
        return pltpu.make_async_remote_copy(
            src_ref=src, dst_ref=dst, send_sem=ssem, recv_sem=rsem,
            device_id=(ep, tp), device_id_type=MESH,
        )

    barrier = pltpu.get_barrier_semaphore()
    for d in range(1, E):
        pl.semaphore_signal(barrier, inc=1, device_id=(ep_at(d), mt), device_id_type=MESH)
    for d in range(1, T):
        pl.semaphore_signal(barrier, inc=1, device_id=(me, tp_at(d)), device_id_type=MESH)

    small = [
        pltpu.make_async_copy(h, v, local_sem.at[i])
        for i, (h, v) in enumerate(
            ((group_h, group_v), (member_h, member_v), (probs_h, probs_v),
             (tokens_h, tokens_v), (gain_h, gain_v), (bias_h, bias_v))
        )
    ]
    for c in small:
        c.start()
    weights = [
        [pltpu.make_async_copy(h.at[j], v.at[j], weight_sem.at[w, j]) for j in range(LE)]
        for w, (h, v) in enumerate(((gate_h, gate_v), (up_h, up_v), (down_h, down_v)))
    ]
    for w in range(2):
        for j in range(LE):
            weights[w][j].start()
    for j in range(LE):
        weights[2][j].start()
    for c in small:
        c.wait()

    lane = iota((n, n), 1)
    sub = iota((n, n), 0)

    def column(row):
        wide = jnp.broadcast_to(row, (n, n))
        return jnp.sum(jnp.where(lane == sub, wide, 0.0), axis=1, keepdims=True)

    group_row = group_v[...].astype(F32)
    group_col = column(group_row)
    same = jnp.where(group_col == group_row, 1.0, 0.0)
    slot_row = jnp.sum(jnp.where(sub < lane, same, 0.0), axis=0, keepdims=True)
    slot_col = jnp.sum(jnp.where(lane < sub, same, 0.0), axis=1, keepdims=True)
    key_row = group_row * cap + slot_row
    key_col = group_col * cap + slot_col
    place = jnp.where(key_row == iota((S, n), 0).astype(F32), 1.0, 0.0)

    def pack(v):
        total = place[:, 0:1] * v[0:1, :]
        for t in range(1, n):
            total += place[:, t : t + 1] * v[t : t + 1, :]
        return total

    probs = probs_v[...]
    member = member_v[...].astype(F32)
    shares = probs / jnp.sum(probs, axis=0, keepdims=True)
    share_lane = iota((n, LANES), 1).astype(F32)
    share_tile = jnp.zeros((n, LANES), F32)
    for k in range(probs.shape[0]):
        hit = share_lane == column(member[k : k + 1, :])
        share_tile += jnp.where(hit, column(shares[k : k + 1, :]), 0.0)
    share_tile = pack(share_tile)
    for g in range(G):
        share_out[g] = share_tile[g * cap : (g + 1) * cap, :]

    values = pack(tokens_v[...].astype(F32))
    center_here = jnp.sum(values, axis=1, keepdims=True) / width
    away = values - center_here
    square_here = jnp.sum(away * away, axis=1, keepdims=True)
    slane = iota((S, LANES), 1)
    stat_buf[0] = jnp.where(slane == 0, center_here, jnp.where(slane == 1, square_here, 0.0))

    pl.semaphore_wait(barrier, E + T - 2)

    stat = [
        remote(stat_buf.at[0], stat_buf.at[d], stat_s.at[d - 1], stat_r.at[d - 1], me, tp_at(d))
        for d in range(1, T)
    ]
    for c in stat:
        c.start()
    share = []
    for d in range(1, E):
        p = ep_at(d)
        c = remote(
            share_out.at[lax.div(p, group_devices)], share_in.at[d],
            share_s.at[d - 1], share_r.at[d - 1], p, mt,
        )
        c.start()
        share.append(c)
    share_in[0] = share_out[lax.div(me, group_devices)]
    gain = gain_v[...]
    bias = bias_v[...]
    for c in stat:
        c.wait_recv()
    stats = [stat_buf[d] for d in range(T)]
    center = sum(s[:, 0:1] for s in stats) / T
    square = sum(s[:, 1:2] + width * (s[:, 0:1] - center) * (s[:, 0:1] - center) for s in stats)
    spread = square / (width * T)
    normed = (values - center) * lax.rsqrt(spread + norm_epsilon) * gain + bias
    for g in range(G):
        rows_out[g] = normed[g * cap : (g + 1) * cap, :].astype(BF16)

    sent = []
    for d in range(1, E):
        p = ep_at(d)
        c = remote(
            rows_out.at[lax.div(p, group_devices)], rows_in.at[d],
            rows_s.at[d - 1], rows_r.at[d - 1], p, mt,
        )
        c.start()
        sent.append(c)
    rows_in[0] = rows_out[lax.div(me, group_devices)]
    rows_all[0:cap, :] = rows_in[0].astype(F32)
    for w in range(2):
        for j in range(LE):
            weights[w][j].wait()
    for d in range(1, E):
        sent[d - 1].wait_recv()
        rows_all[d * cap : (d + 1) * cap, :] = rows_in[d].astype(F32)
    rows = rows_all[...].astype(BF16)

    mine = pl.ds(pl.multiple_of(core * half, half), half)
    theirs = pl.ds(pl.multiple_of((1 - core) * half, half), half)
    partner = my * CORES + (1 - core)
    to_core = []
    for j in range(LE):
        for w, v in enumerate((gate_v, up_v)):
            core_out[j, w] = jnp.dot(rows, v[j, :, theirs], preferred_element_type=F32).astype(BF16)
        c = remote(core_out.at[j], core_in.at[j], core_s.at[j], core_r.at[j], me, partner)
        c.start()
        to_core.append(c)
    to_y = []
    for j in range(LE):
        for w, v in enumerate((gate_v, up_v)):
            held[j, w] = jnp.dot(rows, v[j, :, mine], preferred_element_type=F32)
        to_core[j].wait_recv()
        for w in range(2):
            total = held[j, w] + core_in[j, w].astype(F32)
            held[j, w] = total
            y_out[j, w] = total.astype(BF16)
        copies = []
        for d in range(1, NY):
            c = remote(
                y_out.at[j], y_in.at[j, d - 1], y_s.at[j, d - 1], y_r.at[j, d - 1],
                me, lax.rem(my + d, NY) * CORES + core,
            )
            c.start()
            copies.append(c)
        to_y.append(copies)
    for d in range(1, E):
        share[d - 1].wait_recv()
    for d in range(E):
        share_all[d * cap : (d + 1) * cap, :] = share_in[d]
    for j in range(LE):
        weights[2][j].wait()
    to_hid = []
    partial = []
    for j in range(LE):
        gate = held[j, 0]
        up = held[j, 1]
        for d in range(1, NY):
            to_y[j][d - 1].wait_recv()
            gate += y_in[j, d - 1, 0].astype(F32)
            up += y_in[j, d - 1, 1].astype(F32)
        hidden = (gate / (1.0 + jnp.exp(-gate)) * up).astype(BF16)
        hid_own[j] = hidden
        c = remote(hid_own.at[j], hid_other.at[j], hid_s.at[j], hid_r.at[j], me, partner)
        c.start()
        to_hid.append(c)
        partial.append(jnp.dot(hidden, down_v[j, mine, :], preferred_element_type=F32))
    total = jnp.zeros((R, width), F32)
    rlane = iota((R, LANES), 1)
    weight_tile = share_all[...]
    for j in range(LE):
        to_hid[j].wait_recv()
        expert = partial[j] + jnp.dot(hid_other[j], down_v[j, theirs, :], preferred_element_type=F32)
        which = lax.rem(me * LE + j, EPG)
        weight = jnp.sum(jnp.where(rlane == which, weight_tile, 0.0), axis=1, keepdims=True)
        total += weight * expert.astype(BF16).astype(F32)

    back = []
    for d in range(1, E):
        back_out[d] = total[d * cap : (d + 1) * cap, :].astype(BF16)
        c = remote(
            back_out.at[d], back_in.at[me], back_s.at[d - 1], back_r.at[d - 1],
            lax.rem(me - d + E, E), mt,
        )
        c.start()
        back.append(c)
    back_in[me] = total[0:cap, :].astype(BF16)
    for c in stat:
        c.wait_send()
    for c in share:
        c.wait_send()
    for c in sent:
        c.wait_send()
    for j in range(LE):
        to_core[j].wait_send()
        to_hid[j].wait_send()
        for c in to_y[j]:
            c.wait_send()
    for c in back:
        c.wait()
    finder = jnp.where(key_col == iota((n, LANES), 1).astype(F32), 1.0, 0.0)
    mixed = jnp.zeros((n, width), F32)
    for g in range(G):
        part = back_in[g * group_devices].astype(F32)
        for p in range(1, group_devices):
            part += back_in[g * group_devices + p].astype(F32)
        for s in range(cap):
            at = g * cap + s
            mixed += finder[:, at : at + 1] * part[s : s + 1, :]
    out_ref[...] = mixed


def per_device(E, T, tokens, norm_gain, norm_bias, group_pick, member_pick, picked_probs,
               gate_weight, up_weight, down_weight):
    n, width = tokens.shape
    LE, _, FF = gate_weight.shape
    half = FF // CORES
    NY = T // CORES
    G = LE * E // EPG
    cap = max(n // 4, (n + G - 1) // G)
    S = G * cap
    R = E * cap
    k = picked_probs.shape[1]
    dma = pltpu.SemaphoreType.DMA
    V = pltpu.VMEM
    scratch = [
        V((n, width), BF16), V((1, width), F32), V((1, width), F32),
        V((1, n), jnp.int32), V((k, n), jnp.int32), V((k, n), F32),
        V((LE, width, FF), BF16), V((LE, width, FF), BF16), V((LE, FF, width), BF16),
        V((T, S, LANES), F32),
        V((G, cap, LANES), F32), V((E, cap, LANES), F32), V((R, LANES), F32),
        V((G, cap, width), BF16), V((E, cap, width), BF16), V((R, width), F32),
        V((LE, 2, R, half), BF16), V((LE, 2, R, half), BF16),
        V((LE, 2, R, half), BF16), V((LE, NY - 1, 2, R, half), BF16),
        V((LE, 2, R, half), F32),
        V((LE, R, half), BF16), V((LE, R, half), BF16),
        V((E, cap, width), BF16), V((E, cap, width), BF16),
        dma((6,)), dma((3, LE)),
        dma((T - 1,)), dma((T - 1,)), dma((E - 1,)), dma((E - 1,)), dma((E - 1,)), dma((E - 1,)),
        dma((LE,)), dma((LE,)), dma((LE, NY - 1)), dma((LE, NY - 1)), dma((LE,)), dma((LE,)),
        dma((E - 1,)), dma((E - 1,)),
    ]
    anywhere = pl.BlockSpec(memory_space=pl.ANY)
    combined = pl.pallas_call(
        functools.partial(kernel, E, T, G, cap),
        out_shape=jax.ShapeDtypeStruct((n, width), F32),
        in_specs=[anywhere] * 9,
        out_specs=pl.BlockSpec(memory_space=pltpu.VMEM),
        scratch_shapes=scratch,
        compiler_params=pltpu.CompilerParams(collective_id=0, has_side_effects=True),
        name="moe_step",
    )(tokens, norm_gain.reshape(1, width), norm_bias.reshape(1, width), group_pick.T, member_pick.T,
      picked_probs.T, gate_weight, up_weight, down_weight)
    return combined.astype(BF16)


def solution(mesh):
    placed = (
        P("ep", "tp"), P("tp"), P("tp"), P("ep", None), P("ep", None), P("ep", None),
        P("ep", "tp", None), P("ep", "tp", None), P("ep", None, "tp"),
    )
    body = functools.partial(per_device, mesh.shape["ep"], mesh.shape["tp"])
    return jax.shard_map(body, mesh=mesh, in_specs=placed, out_specs=P("ep", "tp"), check_vma=False)
```
